32 devices in a mesh: grp: 2 (over y), kv: 4 (over z), tp: 4 (over x, core).
Axes of the slice: x: 2, y: 2, z: 4, core: 2. Of those that a mesh axis runs over, the one named last changes fastest.
Arguments:
- tokens: bfloat16 [64, 4096], P('grp', ('kv', 'tp')), parts along dimension 0, may hold values from -12 to 12
- gain_in: float32 [4096], P('kv'), may hold values from 0.1 to 1.9
- w_query: bfloat16 [4096, 1024], P('kv', 'tp'), may hold values from -0.09375 to 0.09375
- w_key: bfloat16 [4096, 1024], P('kv', 'tp'), may hold values from -0.09375 to 0.09375
- w_value: bfloat16 [4096, 2048], P('kv', 'tp'), may hold values from -0.09375 to 0.09375
- w_outgate: bfloat16 [4096, 2048], P('kv', 'tp'), may hold values from -0.09375 to 0.09375
- w_input_gate: bfloat16 [4096, 16], P('kv'), may hold values from -0.09375 to 0.09375
- w_forget_gate: bfloat16 [4096, 16], P('kv'), may hold values from -0.09375 to 0.09375
- bias_input: float32 [16], replicated, may hold values from -1 to 1
- bias_forget: float32 [16], replicated, may hold values from -1 to 4
- cell_state: float32 [64, 16, 64, 128], P(('grp', 'kv'), 'tp'), parts along dimension 0, may hold values from -6 to 6
- norm_state: float32 [64, 16, 64], P(('grp', 'kv'), 'tp'), parts along dimension 0, may hold values from -18 to 18
- max_state: float32 [64, 16], P(('grp', 'kv'), 'tp'), parts along dimension 0, may hold values from -1 to 2
- w_proj: bfloat16 [2048, 4096], P('tp', 'kv'), may hold values from -0.125 to 0.125
- gain_mid: float32 [4096], P('kv'), may hold values from 0.1 to 1.9
- w_up: bfloat16 [4096, 16384], P('kv', 'tp'), may hold values from -0.09375 to 0.09375
- w_down: bfloat16 [16384, 4096], P('tp', 'kv'), may hold values from -0.046875 to 0.046875
Outputs:
- mixed: bfloat16 [64, 4096], P('grp', ('kv', 'tp')), parts along dimension 0
- cell_new: float32 [64, 16, 64, 128], P(('grp', 'kv'), 'tp'), parts along dimension 0
- norm_new: float32 [64, 16, 64], P(('grp', 'kv'), 'tp'), parts along dimension 0
- max_new: float32 [64, 16], P(('grp', 'kv'), 'tp'), parts along dimension 0
The draws below stay inside these ranges and needn't reach their ends.
There are 2 independent parts, one for each index of `grp`. The reference program is written for one: setup_inputs(seed, part) draws one part's arguments, and reference() takes and returns one part's arrays. A program takes and returns all parts, laid end to end along the dimension named above; an argument that names none is the same for every part. Nothing has to cross between parts.
All inputs are finite; a program needn't handle non-finite values.
Results may differ from the reference program's by a relative error of at most 0.015.
Values may be sent and summed in bfloat16 or wider, within the bound.
A program may use at most 64 MiB of HBM per device.

```python
import math
import jax
import jax.numpy as jnp
from jax import lax

D = 4096
NH = 16
DQK = 64
DV = 128
FF = 16384
BATCH = 32


def draw_tokens(key, part):
    key_scale = jax.random.fold_in(key, 11)
    key_base = jax.random.fold_in(key, 12)
    scales = jnp.exp(jax.random.uniform(key_scale, (16,), jnp.float32, math.log(0.3), math.log(3.0)))
    base = jnp.clip(jax.random.normal(key_base, (BATCH, D), jnp.float32), -4.0, 4.0)
    return (base * jnp.repeat(scales, D // 16)[None, :]).astype(jnp.bfloat16)


def block_levels(key, dims, pieces, smallest, top_value):
    level = 1.0
    for position, parts in pieces:
        draws = jax.random.uniform(jax.random.fold_in(jax.random.fold_in(key, 6), position), (parts,), jnp.float32, smallest / len(pieces), top_value / len(pieces))
        level = level * jnp.repeat(jnp.exp(draws), dims[position] // parts).reshape((-1,) + (1,) * (len(dims) - 1 - position))
    return level


def scatter_about(rng, extent, spread, limit, split=(), dtype=jnp.bfloat16):
    gain = block_levels(rng, extent, split, -0.22, 0.18) if split else 1.0
    array = jax.random.normal(rng, extent, jnp.float32) * spread * gain
    return jnp.minimum(jnp.maximum(array, -limit), limit).astype(dtype)


def setup_inputs(seed: int = 0, part: int = 0) -> dict:
    streams_of = jax.random.split(jax.random.key(seed), 18)
    own_keys = jax.random.split(jax.random.fold_in(streams_of[17], part), 18)
    return {
        "tokens": draw_tokens(jax.random.fold_in(jax.random.fold_in(streams_of[17], part), 71), part),
        "gain_in": jnp.clip(1.0 + 0.18 * jax.random.normal(streams_of[1], (D,), jnp.float32), 0.1, 1.9),
        "w_query": scatter_about(streams_of[2], (D, NH * DQK), D ** -0.5, 0.09375, ((0, 4), (1, 4))),
        "w_key": scatter_about(streams_of[3], (D, NH * DQK), D ** -0.5, 0.09375, ((0, 4), (1, 4))),
        "w_value": scatter_about(streams_of[4], (D, NH * DV), D ** -0.5, 0.09375, ((0, 4), (1, 4))),
        "w_outgate": scatter_about(streams_of[5], (D, NH * DV), D ** -0.5, 0.09375, ((0, 4), (1, 4))),
        "w_input_gate": scatter_about(streams_of[6], (D, NH), D ** -0.5, 0.09375, ((0, 4),)),
        "w_forget_gate": scatter_about(streams_of[7], (D, NH), D ** -0.5, 0.09375, ((0, 4),)),
        "bias_input": jnp.clip(jax.random.uniform(streams_of[8], (NH,), jnp.float32, -1.0, 1.0), -1.0, 1.0),
        "bias_forget": jnp.clip(jax.random.uniform(streams_of[9], (NH,), jnp.float32, -1.0, 4.0), -1.0, 4.0),
        "cell_state": scatter_about(own_keys[10], (BATCH, NH, DQK, DV), 1.0, 6.0, ((0, 4), (1, 4)), jnp.float32),
        "norm_state": scatter_about(own_keys[11], (BATCH, NH, DQK), 3.0, 18.0, ((0, 4), (1, 4)), jnp.float32),
        "max_state": jnp.clip(-1.0 + 3.0 * jax.random.uniform(own_keys[12], (BATCH, NH), jnp.float32) ** block_levels(own_keys[12], (BATCH, NH), ((0, 4), (1, 4)), -0.2, 0.2), -1.0, 2.0),
        "w_proj": scatter_about(streams_of[13], (NH * DV, D), (NH * DV) ** -0.5, 0.125, ((0, 4), (1, 4))),
        "gain_mid": jnp.clip(1.0 + 0.18 * jax.random.normal(streams_of[14], (D,), jnp.float32), 0.1, 1.9),
        "w_up": scatter_about(streams_of[15], (D, FF), D ** -0.5, 0.09375, ((0, 4), (1, 4))),
        "w_down": scatter_about(streams_of[16], (FF, D), FF ** -0.5, 0.046875, ((0, 4), (1, 4))),
    }


EPSILON = 1e-06

def memory_step(query, keys, values, outgate, log_input, log_forget, cell_state, norm_state, max_state):
    max_new = jnp.maximum(log_forget + max_state, log_input)
    keep = jnp.exp(log_forget + max_state - max_new)
    write = jnp.exp(log_input - max_new)
    cell_new = keep[..., None, None] * cell_state + (write[..., None] * keys)[..., :, None] * values[..., None, :]
    norm_new = keep[..., None] * norm_state + write[..., None] * keys
    numer = jnp.einsum('shk,shkv->shv', query, cell_new, precision=lax.Precision.HIGHEST)
    denom = jnp.maximum(jnp.abs(lax.optimization_barrier(jnp.sum(query * norm_new, axis=-1))), jnp.exp(-max_new))
    heads = (jax.nn.sigmoid(outgate) * numer / denom[..., None]).astype(jnp.bfloat16)
    return (heads, cell_new, norm_new, max_new)

def reference(tokens, gain_in, w_query, w_key, w_value, w_outgate, w_input_gate, w_forget_gate, bias_input, bias_forget, cell_state, norm_state, max_state, w_proj, gain_mid, w_up, w_down):
    rows = tokens.shape[0]
    widef = tokens.astype(jnp.float32)
    scale_in = lax.rsqrt(lax.optimization_barrier(jnp.sum(widef * widef, axis=1)) / D + EPSILON)
    normed = (widef * gain_in).astype(jnp.bfloat16)

    def project(weight):
        return jnp.dot(normed, weight, preferred_element_type=jnp.float32) * scale_in[:, None]
    query = project(w_query).reshape(rows, NH, DQK) * DQK ** (-0.5)
    keys = project(w_key).reshape(rows, NH, DQK)
    values = project(w_value).reshape(rows, NH, DV)
    outgate = project(w_outgate).reshape(rows, NH, DV)
    log_input = project(w_input_gate) + bias_input
    log_forget = jax.nn.log_sigmoid(project(w_forget_gate) + bias_forget)
    heads, cell_new, norm_new, max_new = memory_step(query, keys, values, outgate, log_input, log_forget, cell_state, norm_state, max_state)
    branch = jnp.dot(heads.reshape(rows, NH * DV), w_proj, preferred_element_type=jnp.float32)
    middle = (widef + branch).astype(jnp.bfloat16)
    midf = middle.astype(jnp.float32)
    scale_mid = lax.rsqrt(lax.optimization_barrier(jnp.sum(midf * midf, axis=1)) / D + EPSILON)
    normed_mid = (midf * gain_mid).astype(jnp.bfloat16)
    upward = jnp.dot(normed_mid, w_up, preferred_element_type=jnp.float32) * scale_mid[:, None]
    hidden = jnp.square(jax.nn.relu(upward)).astype(jnp.bfloat16)
    down = jnp.dot(hidden, w_down, preferred_element_type=jnp.float32)
    mixed = (midf + down).astype(jnp.bfloat16)
    return (mixed, cell_new, norm_new, max_new)
```

```python
import functools

import jax
import jax.numpy as jnp
from jax import lax
from jax.experimental import pallas as pl
from jax.experimental.pallas import tpu as pltpu
from jax.sharding import PartitionSpec as P

MESH = pl.DeviceIdType.MESH
BF16 = jnp.bfloat16
F32 = jnp.float32

EPSILON = 1e-06


def memory_step(
    query, keys, values, outgate, log_input, log_forget, cell_state, norm_state, max_state
):
    max_new = jnp.maximum(log_forget + max_state, log_input)
    keep = jnp.exp(log_forget + max_state - max_new)
    write = jnp.exp(log_input - max_new)
    cell_new = (
        keep[..., None, None] * cell_state
        + (write[..., None] * keys)[..., :, None] * values[..., None, :]
    )
    norm_new = keep[..., None] * norm_state + write[..., None] * keys
    numer = jnp.einsum("shk,shkv->shv", query, cell_new, precision=lax.Precision.HIGHEST)
    denom = jnp.maximum(jnp.abs(jnp.sum(query * norm_new, axis=-1)), jnp.exp(-max_new))
    heads = (jax.nn.sigmoid(outgate) * numer / denom[..., None]).astype(jnp.bfloat16)
    return (heads, cell_new, norm_new, max_new)


def matmul(left, right):
    return jnp.dot(left, right, preferred_element_type=jnp.float32)


def plain_on_device(
    tokens,
    gain_in,
    w_query,
    w_key,
    w_value,
    w_outgate,
    w_input_gate,
    w_forget_gate,
    bias_input,
    bias_forget,
    cell_state,
    norm_state,
    max_state,
    w_proj,
    gain_mid,
    w_up,
    w_down,
):
    seq_local, head_count = (cell_state.shape[0], cell_state.shape[1])
    key_dim, value_dim = (cell_state.shape[2], cell_state.shape[3])
    head_start = lax.axis_index("tp") * head_count
    column_width = tokens.shape[1]
    D = gain_in.shape[0] * lax.axis_size("kv")
    gathered = lax.all_gather(tokens, "tp", axis=1, tiled=True)
    widef = gathered.astype(jnp.float32)
    part_squares = jnp.sum(widef * widef, axis=1)
    normed = (widef * gain_in).astype(jnp.bfloat16)
    gate_input = lax.dynamic_slice_in_dim(w_input_gate, head_start, head_count, 1)
    gate_forget = lax.dynamic_slice_in_dim(w_forget_gate, head_start, head_count, 1)
    terms = jnp.concatenate(
        [
            matmul(normed, w_query),
            matmul(normed, w_key),
            matmul(normed, w_value),
            matmul(normed, w_outgate),
            matmul(normed, gate_input),
            matmul(normed, gate_forget),
        ],
        axis=1,
    )
    total_squares = lax.psum(part_squares, "kv")
    own_terms = lax.psum_scatter(terms, "kv", scatter_dimension=0, tiled=True)
    row_squares = lax.dynamic_slice_in_dim(
        total_squares, lax.axis_index("kv") * seq_local, seq_local, 0
    )
    own_terms = own_terms * lax.rsqrt(row_squares / D + EPSILON)[:, None]
    width_qk = head_count * key_dim
    width_v = head_count * value_dim
    query = own_terms[:, :width_qk].reshape(seq_local, head_count, key_dim) * key_dim ** (-0.5)
    keys = own_terms[:, width_qk : 2 * width_qk].reshape(seq_local, head_count, key_dim)
    offset = 2 * width_qk
    values = own_terms[:, offset : offset + width_v].reshape(seq_local, head_count, value_dim)
    offset = offset + width_v
    outgate = own_terms[:, offset : offset + width_v].reshape(seq_local, head_count, value_dim)
    offset = offset + width_v
    log_input = own_terms[:, offset : offset + head_count] + lax.dynamic_slice_in_dim(
        bias_input, head_start, head_count, 0
    )
    offset = offset + head_count
    log_forget = jax.nn.log_sigmoid(
        own_terms[:, offset : offset + head_count]
        + lax.dynamic_slice_in_dim(bias_forget, head_start, head_count, 0)
    )
    heads, cell_new, norm_new, max_new = memory_step(
        query, keys, values, outgate, log_input, log_forget, cell_state, norm_state, max_state
    )
    branch_part = matmul(
        lax.all_gather(heads.reshape(seq_local, width_v), "kv", axis=0, tiled=True), w_proj
    )
    branch = lax.psum(branch_part, "tp")
    middle = (widef + branch).astype(jnp.bfloat16)
    midf = middle.astype(jnp.float32)
    mid_squares = jnp.sum(midf * midf, axis=1)
    normed_mid = (midf * gain_mid).astype(jnp.bfloat16)
    up_part = matmul(normed_mid, w_up)
    up_rows, square_rows = (
        lax.psum_scatter(up_part, "kv", scatter_dimension=0, tiled=True),
        lax.psum_scatter(mid_squares, "kv", scatter_dimension=0, tiled=True),
    )
    upward = up_rows * lax.rsqrt(square_rows / D + EPSILON)[:, None]
    hidden = jnp.square(jax.nn.relu(upward)).astype(jnp.bfloat16)
    down_part = matmul(lax.all_gather(hidden, "kv", axis=0, tiled=True), w_down)
    own_down = lax.psum_scatter(
        down_part.astype(jnp.bfloat16), "tp", scatter_dimension=1, tiled=True
    ).astype(jnp.float32)
    residual = lax.dynamic_slice_in_dim(midf, lax.axis_index("tp") * column_width, column_width, 1)
    mixed = (residual + own_down).astype(jnp.bfloat16)
    return (mixed, cell_new, norm_new, max_new)


def matmul_nt(left, right):
    return lax.dot_general(left, right, (((1,), (1,)), ((), ())), preferred_element_type=F32)


def partners(me, count):
    both = [3 - me, lax.rem(me + 2, 4), me + 1 - 2 * lax.rem(me, 2)]
    return both, both


class Link:
    def __init__(self, send_sem, recv_sem):
        self.send_sem, self.recv_sem = send_sem, recv_sem
        self.sent, self.used = 0, 0

    def phase(self):
        index = self.sent
        self.sent += 1
        return self.send_sem.at[index]

    def slot(self):
        index = self.used
        self.used += 1
        return self.recv_sem.at[index]


def remote(src, dst, send, recv, where):
    return pltpu.make_async_remote_copy(
        src_ref=src,
        dst_ref=dst,
        send_sem=send,
        recv_sem=recv,
        device_id=where,
        device_id_type=MESH,
    )


def semaphore_counts(subs):
    return 12, 10, 10 + 3 * subs


def layer_kernel(
    kv,
    tp,
    subs,
    tokens,
    gain_in,
    w_query,
    w_key,
    w_value,
    w_outgate,
    w_input_gate,
    w_forget_gate,
    bias_input,
    bias_forget,
    cell_state,
    norm_state,
    max_state,
    w_proj,
    gain_mid,
    w_up,
    w_down,
    out_v,
    cell_o,
    norm_o,
    max_o,
    tok,
    gain1,
    wqkv,
    wg,
    bias,
    cell,
    norm,
    mstate,
    wproj,
    gain2,
    wup,
    wdown,
    terms,
    b_send,
    b_recv,
    g_send,
    g_recv,
    numer,
    h_all,
    e_all,
    sq_all,
    mid,
    nmid,
    f_own,
    f_send,
    f_recv,
    hid,
    down,
    d_send,
    d_recv,
    in_sem,
    send_sem,
    recv_sem,
):
    k_me, t_me = lax.axis_index("kv"), lax.axis_index("tp")
    core = lax.rem(t_me, 2)
    mate = t_me + 1 - 2 * core
    link = Link(send_sem, recv_sem)
    rows, width = tok.shape[1], tok.shape[2]
    own_rows, n_heads, key_dim, value_dim = cell.shape
    wide = tp * width
    total_width = kv * wide
    w_qk, w_v = n_heads * key_dim, n_heads * value_dim
    n_gates = bias.shape[2]
    half = f_own.shape[2]
    block = subs * half
    half_wide = wide // 2

    groups = [0]

    def load(*pairs):
        sem = in_sem.at[groups[0]]
        groups[0] += 1
        for src, dst in pairs:
            pltpu.make_async_copy(src, dst, sem).start()
        return sem

    def loaded(sem, whole):
        pltpu.make_async_copy(whole, whole, sem).wait()

    def columns(first, size):
        return pl.ds(pl.multiple_of(first, size), size)

    l_tok = load((tokens, tok.at[t_me]))
    l_gain = load((gain_in, gain1))
    l_gates = load((w_input_gate, wg.at[0:n_gates]), (w_forget_gate, wg.at[n_gates : 2 * n_gates]))
    l_qkv = load(
        (w_query, wqkv.at[:, 0:w_qk]),
        (w_key, wqkv.at[:, w_qk : 2 * w_qk]),
        (w_value, wqkv.at[:, 2 * w_qk : 2 * w_qk + w_v]),
        (w_outgate, wqkv.at[:, 2 * w_qk + w_v : 2 * w_qk + 2 * w_v]),
    )
    l_bias = load((bias_input, bias.at[0]), (bias_forget, bias.at[1]))
    l_norm = load((norm_state, norm))
    l_max = load((max_state, mstate))

    barrier = pltpu.get_barrier_semaphore()
    k_peers, k_from = partners(k_me, kv)
    t_far = [3 - t_me, lax.rem(t_me + 2, tp)]
    t_peers = t_far + [mate]
    everyone = [{"tp": p} for p in t_peers] + [{"kv": p} for p in k_peers]
    everyone += [{"kv": p, "tp": mate} for p in k_peers]
    for where in everyone:
        pl.semaphore_signal(barrier, inc=1, device_id=where, device_id_type=MESH)
    loaded(l_tok, tok.at[t_me])
    pl.semaphore_wait(barrier, len(everyone))

    a_sent, a_far, a_mate = link.phase(), link.slot(), link.slot()
    for p in t_far:
        remote(tok.at[t_me], tok.at[t_me], a_sent, a_far, {"tp": p}).start()
    remote(tok.at[t_me], tok.at[t_me], a_sent, a_mate, {"tp": mate}).start()
    w_sent, w_got = link.phase(), link.slot()
    proj_rows = wproj.at[columns(core * w_v, w_v)]
    remote(
        w_proj.at[:, columns((1 - core) * half_wide, half_wide)],
        proj_rows,
        w_sent,
        w_got,
        {"tp": mate},
    ).start()
    l_cell = load((cell_state, cell))
    l_proj = load((w_proj.at[:, columns(core * half_wide, half_wide)], proj_rows))
    l_gain2 = load((gain_mid, gain2))
    spans = [pl.ds(i * (wup.shape[0] // kv), wup.shape[0] // kv) for i in range(kv)]
    l_up = load(*[(w_up.at[s], wup.at[s]) for s in spans])
    spans = [pl.ds(i * block, block) for i in range(kv)]
    l_down = load(*[(w_down.at[s], wdown.at[s]) for s in spans])
    loaded(l_gain, gain1)
    loaded(l_gates, wg)
    loaded(l_qkv, wqkv)

    def normed_tile(t):
        here = columns(t * width, width)
        tile = tok[t].astype(F32)
        squares = jnp.sum(tile * tile, axis=1, keepdims=True)
        tile = (tile * gain1[:, here]).astype(BF16)
        return tile, squares, matmul_nt(tile, wg[:, here]), here

    n_qkv = wqkv.shape[1]
    flat = (kv, own_rows, n_qkv)
    tile, squares, gate_sum, here = normed_tile(t_me)
    terms[...] = matmul(tile, wqkv[here, :]).reshape(flat)
    remote(tok.at[0], tok.at[0], a_sent, a_mate, {"tp": mate}).wait_recv()
    tile, more, gate_more, here = normed_tile(mate)
    squares, gate_sum = squares + more, gate_sum + gate_more
    terms[...] = terms[...] + matmul(tile, wqkv[here, :]).reshape(flat)
    remote(tok.at[0:2], tok.at[0:2], a_sent, a_far, {"tp": mate}).wait_recv()
    far = [normed_tile(t) for t in t_far]
    for _, more, gate_more, _ in far:
        squares, gate_sum = squares + more, gate_sum + gate_more
    packed = jnp.concatenate(
        [gate_sum, jnp.broadcast_to(squares, (rows, 128 - 2 * n_gates))], axis=1
    )
    g_send[...] = packed.reshape(kv, own_rows, 128)
    g_sent, g_got = link.phase(), link.slot()
    for o, p in enumerate(k_peers):
        remote(g_send.at[p], g_recv.at[o], g_sent, g_got, {"kv": p}).start()
    b_sent, b_got = link.phase(), []
    pieces = (slice(0, n_qkv // 2), slice(n_qkv // 2, n_qkv))
    for cols in pieces:
        size = cols.stop - cols.start
        part = terms[:, :, cols]
        for tile, _, _, here in far:
            part = part + matmul(tile, wqkv[here, cols]).reshape(kv, own_rows, size)
        terms[:, :, cols] = part
        b_send[:, :, cols] = part.astype(BF16)
        got = link.slot()
        b_got.append(got)
        for o, p in enumerate(k_peers):
            remote(
                b_send.at[p, :, cols], b_recv.at[o, :, cols], b_sent, got, {"kv": p}
            ).start()

    loaded(l_bias, bias)
    loaded(l_norm, norm)
    loaded(l_max, mstate)
    loaded(l_cell, cell)
    near_kv = {"kv": k_peers[2]}
    remote(g_recv, g_recv, g_sent, g_got, near_kv).wait_recv()
    gates = g_send[k_me]
    for o in range(kv - 1):
        gates = gates + g_recv[o]
    scale = lax.rsqrt(gates[:, 2 * n_gates : 2 * n_gates + 1] / total_width + EPSILON)
    log_i = gates[:, 0:n_gates] * scale + bias[0]
    raw_f = gates[:, n_gates : 2 * n_gates] * scale + bias[1]
    log_f = jnp.minimum(raw_f, 0.0) - jnp.log1p(jnp.exp(-jnp.abs(raw_f)))
    gate_lane = lax.broadcasted_iota(jnp.int32, (own_rows, n_gates), 1)
    keep, write, floor = [], [], []
    max_cols = []
    old_max = mstate[...].T
    for h in range(n_heads):
        pick = gate_lane == t_me * n_heads + h
        li = jnp.sum(jnp.where(pick, log_i, 0.0), axis=1, keepdims=True)
        lf = jnp.sum(jnp.where(pick, log_f, 0.0), axis=1, keepdims=True)
        old = old_max[:, h : h + 1]
        new = jnp.maximum(lf + old, li)
        max_cols.append(new)
        keep.append(jnp.exp(lf + old - new))
        write.append(jnp.exp(li - new))
        floor.append(jnp.exp(-new))
    head_lane = lax.broadcasted_iota(jnp.int32, (own_rows, n_heads), 1)
    new_max = jnp.broadcast_to(max_cols[0], (own_rows, n_heads))
    for h in range(1, n_heads):
        new_max = jnp.where(head_lane == h, max_cols[h], new_max)
    max_o[...] = new_max.T
    for cols, got in zip(pieces, b_got):
        here = b_recv.at[:, :, cols]
        remote(here, here, b_sent, got, near_kv).wait_recv()
    own = terms[k_me]
    for o in range(kv - 1):
        own = own + b_recv[o].astype(F32)
    own = own * scale
    query = own[:, 0:w_qk] * key_dim ** (-0.5)
    keys = own[:, w_qk : 2 * w_qk]
    values = own[:, 2 * w_qk : 2 * w_qk + w_v]
    outgate = own[:, 2 * w_qk + w_v : 2 * w_qk + 2 * w_v]
    qk_head = lax.broadcasted_iota(jnp.int32, (own_rows, w_qk), 1) // key_dim
    spread = jnp.broadcast_to(write[0], (own_rows, w_qk))
    for h in range(1, n_heads):
        spread = jnp.where(qk_head == h, write[h], spread)
    wkeys = keys * spread
    pad = jnp.zeros((128 - 2 * own_rows, w_qk), F32)
    turned = jnp.concatenate([wkeys, query, pad], axis=0).T
    denom, cross = [], []
    for h in range(n_heads):
        part = slice(h * key_dim, (h + 1) * key_dim)
        fresh = keep[h] * norm[:, h, :] + wkeys[:, part]
        norm_o[:, h, :] = fresh
        dot = jnp.sum(query[:, part] * fresh, axis=1, keepdims=True)
        shape_v = (own_rows, value_dim)
        denom.append(jnp.broadcast_to(jnp.maximum(jnp.abs(dot), floor[h]), shape_v))
        dot = jnp.sum(query[:, part] * wkeys[:, part], axis=1, keepdims=True)
        cross.append(jnp.broadcast_to(dot, shape_v))
    for h in range(n_heads):
        part = slice(h * key_dim, (h + 1) * key_dim)
        vals = slice(h * value_dim, (h + 1) * value_dim)
        for s in range(own_rows):
            q_col = turned[part, own_rows + s : own_rows + s + 1]
            numer[s : s + 1, vals] = jnp.sum(q_col * cell[s, h], axis=0, keepdims=True)
    keep_v = jnp.concatenate(
        [jnp.broadcast_to(one, (own_rows, value_dim)) for one in keep], axis=1
    )
    above = keep_v * numer[...] + jnp.concatenate(cross, axis=1) * values
    heads = jax.nn.sigmoid(outgate) * above / jnp.concatenate(denom, axis=1)
    mine = core * kv + k_me
    h_all[mine] = heads.astype(BF16)
    h_sent, h_got = link.phase(), link.slot()
    targets = [{"kv": p, "tp": t} for p in k_peers for t in (mate, t_me)] + [{"tp": mate}]
    for where in targets:
        remote(h_all.at[mine], h_all.at[mine], h_sent, h_got, where).start()
    for h in range(n_heads):
        part = slice(h * key_dim, (h + 1) * key_dim)
        vals = slice(h * value_dim, (h + 1) * value_dim)
        for s in range(own_rows):
            cell_o[s, h] = (
                keep[h][s : s + 1, :] * cell[s, h]
                + turned[part, s : s + 1] * values[s : s + 1, vals]
            )
    loaded(l_proj, wproj.at[0:w_v])
    remote(wproj.at[0:w_v], wproj.at[0:w_v], w_sent, w_got, {"tp": mate}).wait_recv()
    n_sent = len(targets)
    remote(h_all.at[0:n_sent], h_all.at[0:n_sent], h_sent, h_got, near_kv).wait_recv()
    all_heads = jnp.concatenate(
        [
            jnp.concatenate([h_all[c * kv + i].astype(F32) for i in range(kv)], axis=0)
            for c in range(2)
        ],
        axis=1,
    ).astype(BF16)
    e_all[t_me] = matmul(all_heads, wproj[...]).astype(BF16)
    e_sent, e_got = link.phase(), link.slot()
    for p in t_peers:
        remote(e_all.at[t_me], e_all.at[t_me], e_sent, e_got, {"tp": p}).start()
    loaded(l_gain2, gain2)
    remote(e_all.at[0 : tp - 1], e_all.at[0 : tp - 1], e_sent, e_got, {"tp": mate}).wait_recv()
    branch = jnp.concatenate(
        [
            sum(e_all[i].astype(F32) for i in range(c + 2, tp, 2)) + e_all[c].astype(F32)
            for c in range(2)
        ],
        axis=1,
    )
    wide_f = jnp.concatenate([tok[i] for i in range(tp)], axis=1).astype(F32)
    middle = (wide_f + branch).astype(BF16).astype(F32)
    for i in range(tp):
        mid[i] = middle[:, i * width : (i + 1) * width]
    diagonal = lax.broadcasted_iota(jnp.int32, (rows, 128), 0) == lax.broadcasted_iota(
        jnp.int32, (rows, 128), 1
    )
    row_squares = jnp.sum(middle * middle, axis=1, keepdims=True)
    sq_all[k_me] = jnp.sum(jnp.where(diagonal, row_squares, 0.0), axis=0, keepdims=True)
    s_sent, s_got = link.phase(), link.slot()
    for p in k_peers:
        remote(sq_all.at[k_me], sq_all.at[k_me], s_sent, s_got, {"kv": p}).start()
    nmid[...] = (middle * gain2[...]).astype(BF16)

    loaded(l_up, wup)
    is_end = jnp.logical_or(k_me == 0, k_me == kv - 1)
    is_mid = jnp.logical_not(is_end)
    across, skip, near = k_peers
    targets = [across, jnp.where(is_end, near, skip), near]
    place = (0, 2, 1)
    f_sent = link.phase()
    f_pair, f_skip = [], []
    f_across = []
    for sub in range(subs):
        pair, alone = link.slot(), link.slot()
        f_pair.append(pair)
        f_skip.append(alone)
        for o in (1, 0, 2):
            part = matmul(nmid[...], wup[:, columns(k_peers[o] * block + sub * half, half)])
            f_send[sub, place[o]] = part.astype(BF16)
        f_own[sub] = matmul(nmid[...], wup[:, columns(k_me * block + sub * half, half)])
        for o in (1, 0, 2):
            one = remote(
                f_send.at[sub, place[o]],
                f_recv.at[sub, place[o]],
                f_sent,
                alone if o == 1 else pair,
                {"kv": targets[o]},
            )
            if o:
                one.start()
            else:
                pl.when(is_end)(one.start)
                f_across.append(one)
    remote(sq_all.at[0 : kv - 1], sq_all.at[0 : kv - 1], s_sent, s_got, near_kv).wait_recv()
    row_sum = sq_all[0]
    for i in range(1, kv):
        row_sum = row_sum + sq_all[i]
    row_sum = jnp.sum(jnp.where(diagonal, row_sum, 0.0), axis=1, keepdims=True)
    scale_mid = lax.rsqrt(row_sum / total_width + EPSILON)
    g2_sent, g2_got = link.phase(), []

    def relay(sub):
        here = f_recv.at[sub, 2]
        remote(here, here, f_sent, f_skip[sub], near_kv).wait_recv()

        def add():
            both = f_send[sub, 0].astype(F32) + f_recv[sub, 2].astype(F32)
            f_send[sub, 0] = both.astype(BF16)
            f_across[sub].start()

        pl.when(is_mid)(add)

    def complete(sub):
        here = f_recv.at[sub, 0:2]
        remote(here, here, f_sent, f_pair[sub], near_kv).wait_recv()
        upward = f_own[sub]
        skipped = jnp.where(is_end, f_recv[sub, 2].astype(F32), 0.0)
        upward = upward + f_recv[sub, 0].astype(F32) + skipped + f_recv[sub, 1].astype(F32)
        hid[k_me, sub] = jnp.square(jnp.maximum(upward * scale_mid, 0.0)).astype(BF16)
        mine = hid.at[k_me, sub]
        got = link.slot()
        g2_got.append(got)
        for peer in k_peers:
            remote(mine, mine, g2_sent, got, {"kv": peer}).start()

    ahead = 2
    for sub in range(subs):
        relay(sub)
        if sub >= ahead:
            complete(sub - ahead)
    for sub in range(subs - min(ahead, subs), subs):
        complete(sub)

    loaded(l_down, wdown)

    def lower(source, sub):
        return matmul(hid[source, sub], wdown[columns(source * block + sub * half, half), :])

    part = lower(k_me, 0)
    for sub in range(1, subs):
        part = part + lower(k_me, sub)
    down[...] = part
    for sub in range(subs):
        here = hid.at[0 : kv - 1, sub]
        remote(here, here, g2_sent, g2_got[sub], near_kv).wait_recv()
        part = down[...]
        for o in (2, 1, 0):
            part = part + lower(k_from[o], sub)
        down[...] = part
    for i in range(tp):
        d_send[i] = down[:, i * width : (i + 1) * width].astype(BF16)
    d_sent, d_got = link.phase(), link.slot()
    for o, p in enumerate(t_peers):
        remote(d_send.at[p], d_recv.at[o], d_sent, d_got, {"tp": p}).start()
    own_part = d_send[t_me].astype(F32)
    remote(d_recv, d_recv, d_sent, d_got, {"tp": mate}).wait_recv()
    for o in range(tp - 1):
        own_part = own_part + d_recv[o].astype(F32)
    out_v[...] = (mid[t_me] + own_part).astype(BF16)
    for sem, whole in (
        (a_sent, tok.at[0 : tp - 1]),
        (w_sent, wproj.at[0:w_v]),
        (g_sent, g_recv),
        (b_sent, b_recv),
        (h_sent, h_all.at[0:n_sent]),
        (e_sent, e_all.at[0 : tp - 1]),
        (s_sent, sq_all.at[0 : kv - 1]),
        (f_sent, f_recv),
        (g2_sent, hid.at[0 : kv - 1]),
        (d_sent, d_recv),
    ):
        remote(whole, whole, sem, b_got[0], near_kv).wait_send()


def finish_kernel(*refs):
    sources, outs, sem = refs[0:4], refs[4:8], refs[8]
    copies = [pltpu.make_async_copy(sources[i], outs[i], sem.at[i]) for i in range(4)]
    for one in copies:
        one.start()
    for one in copies:
        one.wait()


def fused_on_device(kv, tp, *args):
    (tokens, gain_in, w_query, w_key, w_value, w_outgate, w_input_gate, w_forget_gate) = args[:8]
    (bias_input, bias_forget, cell_state, norm_state, max_state) = args[8:13]
    (w_proj, gain_mid, w_up, w_down) = args[13:]
    rows, width = tokens.shape
    own_rows = cell_state.shape[0]
    wide = w_query.shape[0]
    n_qkv = w_query.shape[1] + w_key.shape[1] + w_value.shape[1] + w_outgate.shape[1]
    hidden = w_up.shape[1]
    subs = 4 if hidden % (1024 * kv) == 0 else 2
    half = hidden // (kv * subs)
    w_v = w_value.shape[1]
    operands = tuple(pltpu.with_memory_space_constraint(x, pltpu.HBM) for x in (
        tokens,
        gain_in.reshape(1, -1),
        w_query,
        w_key,
        w_value,
        w_outgate,
        w_input_gate.T,
        w_forget_gate.T,
        bias_input.reshape(1, -1),
        bias_forget.reshape(1, -1),
        cell_state,
        norm_state,
        max_state.T,
        w_proj,
        gain_mid.reshape(1, -1),
        w_up,
        w_down,
    ))
    n_in, n_send, n_recv = semaphore_counts(subs)
    n_gates = w_input_gate.shape[1]
    vm = pltpu.VMEM
    scratch = [
        vm((tp, rows, width), BF16),
        vm((1, wide), F32),
        vm((wide, n_qkv), BF16),
        vm((2 * n_gates, wide), BF16),
        vm((2, 1, n_gates), F32),
        vm(cell_state.shape, F32),
        vm(norm_state.shape, F32),
        vm(max_state.shape[::-1], F32),
        vm((2 * w_v, wide // 2), BF16),
        vm((1, wide), F32),
        vm(w_up.shape, BF16),
        vm(w_down.shape, BF16),
        vm((kv, own_rows, n_qkv), F32),
        vm((kv, own_rows, n_qkv), BF16),
        vm((kv - 1, own_rows, n_qkv), BF16),
        vm((kv, own_rows, 128), F32),
        vm((kv - 1, own_rows, 128), F32),
        vm((own_rows, w_v), F32),
        vm((2 * kv, own_rows, w_v), BF16),
        vm((tp, rows, wide // 2), BF16),
        vm((kv, 1, 128), F32),
        vm((tp, rows, width), F32),
        vm((rows, wide), BF16),
        vm((subs, rows, half), F32),
        vm((subs, kv - 1, rows, half), BF16),
        vm((subs, kv - 1, rows, half), BF16),
        vm((kv, subs, rows, half), BF16),
        vm((rows, wide), F32),
        vm((tp, rows, width), BF16),
        vm((tp - 1, rows, width), BF16),
        pltpu.SemaphoreType.DMA((n_in,)),
        pltpu.SemaphoreType.DMA((n_send,)),
        pltpu.SemaphoreType.DMA((n_recv,)),
    ]
    anywhere = pl.BlockSpec(memory_space=pltpu.HBM)
    in_vmem = pl.BlockSpec(memory_space=pltpu.VMEM)
    results = pl.pallas_call(
        functools.partial(layer_kernel, kv, tp, subs),
        out_shape=(
            jax.ShapeDtypeStruct((rows, width), BF16),
            jax.ShapeDtypeStruct(cell_state.shape, F32),
            jax.ShapeDtypeStruct(norm_state.shape, F32),
            jax.ShapeDtypeStruct(max_state.shape[::-1], F32),
        ),
        in_specs=[anywhere] * len(operands),
        out_specs=(in_vmem,) * 4,
        scratch_shapes=scratch,
        compiler_params=pltpu.CompilerParams(
            collective_id=0, has_side_effects=True, vmem_limit_bytes=36 * 1024 * 1024
        ),
    )(*operands)
    mixed, cell_new, norm_new, max_new = pl.pallas_call(
        finish_kernel,
        out_shape=tuple(jax.ShapeDtypeStruct(one.shape, one.dtype) for one in results),
        in_specs=[in_vmem] * 4,
        out_specs=(anywhere,) * 4,
        scratch_shapes=[pltpu.SemaphoreType.DMA((4,))],
        compiler_params=pltpu.CompilerParams(vmem_limit_bytes=8 * 1024 * 1024),
    )(*results)
    return (mixed, cell_new, norm_new, max_new.T)


def fits_kernel(kv, tp, *args):
    tokens, w_query, cell_state, w_up = args[0], args[2], args[10], args[15]
    return (
        kv == 4
        and tp == 4
        and tokens.shape[1] % 128 == 0
        and w_query.shape[0] % 256 == 0
        and w_query.shape[1] % 256 == 0
        and args[4].shape[1] % 256 == 0
        and cell_state.shape[0] % 8 == 0
        and 2 * cell_state.shape[0] <= 128
        and cell_state.shape[3] % 128 == 0
        and w_up.shape[1] % (512 * kv) == 0
        and args[6].shape[1] % 16 == 0
        and 2 * args[6].shape[1] < 128
        and tokens.shape[0] <= 128
    )


def on_device(kv, tp, *args):
    if fits_kernel(kv, tp, *args):
        return fused_on_device(kv, tp, *args)
    return plain_on_device(*args)


def solution(mesh):
    in_specs = (
        P("grp", ("kv", "tp")),
        P("kv"),
        P("kv", "tp"),
        P("kv", "tp"),
        P("kv", "tp"),
        P("kv", "tp"),
        P("kv", None),
        P("kv", None),
        P(),
        P(),
        P(("grp", "kv"), "tp", None, None),
        P(("grp", "kv"), "tp", None),
        P(("grp", "kv"), "tp"),
        P("tp", "kv"),
        P("kv"),
        P("kv", "tp"),
        P("tp", "kv"),
    )
    out_specs = (
        P("grp", ("kv", "tp")),
        P(("grp", "kv"), "tp", None, None),
        P(("grp", "kv"), "tp", None),
        P(("grp", "kv"), "tp"),
    )
    return jax.shard_map(
        functools.partial(on_device, mesh.shape["kv"], mesh.shape["tp"]),
        mesh=mesh, in_specs=in_specs, out_specs=out_specs, check_vma=False
    )
```
